32 devices in a mesh: sp: 8 (over z, x), tp: 4 (over y, core).
Axes of the slice: x: 2, y: 2, z: 4, core: 2. Of those that a mesh axis runs over, the one named last changes fastest.
Arguments:
- tokens: bfloat16 [2048, 4096], P('sp', 'tp'), may hold values from -6 to 6
- pre_gain: float32 [4096], replicated, may hold values from 0.1 to 1.9
- rate_factor: float32 [2048], P('sp'), may hold values from 0.5 to 2, as said below
- w_rec_in: bfloat16 [4096, 1024], P(None, 'tp'), may hold values from -0.09375 to 0.09375
- w_rec_gate: bfloat16 [4096, 1024], P(None, 'tp')
- conv_taps: float32 [4, 1024], P(None, 'tp'), may hold values from -3 to 3
- rate_maps: bfloat16 [8, 128, 128], P('tp'), may hold values from -0.5 to 0.5
- input_maps: bfloat16 [8, 128, 128], P('tp'), may hold values from -0.5 to 0.5
- decay_param: float32 [1024], P('tp'), as said below
- w_query: bfloat16 [4096, 1536], P(None, 'tp'), may hold values from -0.09375 to 0.09375
- w_latent: bfloat16 [4096, 512], replicated, may hold values from -0.09375 to 0.09375
- w_rope_key: bfloat16 [4096, 64], replicated, may hold values from -0.09375 to 0.09375
- latent_gain: float32 [512], replicated, may hold values from 0.7 to 100, as said below
- w_expand: bfloat16 [512, 2048], P(None, 'tp')
- rec_gain: float32 [1024], P('tp'), may hold values from 0.1 to 1.9
- att_gain: float32 [1024], P('tp'), may hold values from 0.1 to 1.9
- w_out_rec: bfloat16 [1024, 4096], P('tp'), may hold values from -0.125 to 0.125
- w_out_att: bfloat16 [1024, 4096], P('tp'), may hold values from -0.125 to 0.125
- post_gain: float32 [4096], replicated, may hold values from 0.1 to 1.9
Outputs:
- layer_out: bfloat16 [2048, 4096], P(('sp', 'tp'))
The draws below stay inside these ranges and needn't reach their ends.
Inputs may be any that keep to these rules, and one draw needn't show every extreme that they name: `rate_factor`: one positive factor for each position. `decay_param`: one parameter for each recurrent channel. `latent_gain`: one positive gain for each latent entry.
All inputs are finite; a program needn't handle non-finite values.
Results may differ from the reference program's by a relative error of at most 0.017.
The reference program's roundings to bfloat16 on the way count: a program that leaves them out, or rounds other values in their place, can miss the bound.
Values may be sent and summed in bfloat16 or wider, within the bound.
No kernel may reach another device: no remote copies, remote signals or barrier semaphores. Data moves between devices by JAX's collectives and lax.ppermute only.
A program may use at most 128 MiB of HBM per device.

```python
import math
import jax
import jax.numpy as jnp
from jax import lax

D = 4096
LRU_W = 1024
LRU_BLK = 128
CONV = 4
HEADS = 8
NOPE = 128
ROPE = 64
VDIM = 128
LATENT = 512
TOK_DEV = 256
SEQ = 2048
N_TP = 4


def draw_rate_factor(key, part):
    span_rows = max(TOK_DEV // 2, 1)
    levels = jnp.exp(jax.random.uniform(key, (SEQ // span_rows,), jnp.float32, math.log(0.5), math.log(2.0)))
    return jnp.repeat(levels, span_rows, total_repeat_length=SEQ)


def draw_decay_param(key, part):
    choose_key, slow_key, fast_key = jax.random.split(key, 3)
    share = 0.5
    slow_mask = jax.random.uniform(choose_key, (LRU_W,), jnp.float32) < share
    slow_value = math.log(8.0 * SEQ) + jax.random.uniform(slow_key, (LRU_W,), jnp.float32, 0.5, 2.0)
    fast_value = jax.random.uniform(fast_key, (LRU_W,), jnp.float32, 4.5, 6.0)
    return jnp.where(slow_mask, slow_value, fast_value)


def draw_latent_gain(key, part):
    return jax.random.uniform(key, (LATENT,), jnp.float32, 0.7, 1.3)


def draw_w_rec_gate(key, part):
    base_key, factor_key = jax.random.split(key)
    base = jax.random.normal(base_key, (D, LRU_W), jnp.float32) / math.sqrt(D)
    factors = jnp.exp(jax.random.uniform(factor_key, (LRU_W // LRU_BLK,), jnp.float32, math.log(1.0 / 3.0), math.log(3.0)))
    return (base * jnp.repeat(factors, LRU_BLK, total_repeat_length=LRU_W)[None, :]).astype(jnp.bfloat16)


def draw_w_expand(key, part):
    base_key, factor_key = jax.random.split(key)
    base = jax.random.normal(base_key, (LATENT, HEADS, NOPE + VDIM), jnp.float32) / math.sqrt(LATENT)
    factors = jnp.exp(jax.random.uniform(factor_key, (HEADS,), jnp.float32, math.log(1.0 / 3.0), math.log(3.0)))
    columns = jnp.arange(NOPE + VDIM)
    scaling = jnp.where(columns[None, :] >= NOPE, factors[:, None], 1.0)
    return (base * scaling[None, :, :]).reshape(LATENT, HEADS * (NOPE + VDIM)).astype(jnp.bfloat16)


def level_of(own_key, dims, cuts, low, high):
    level = 1.0
    for dim, shards_of in cuts:
        steps = jax.random.uniform(jax.random.fold_in(jax.random.fold_in(own_key, 6), dim), (shards_of,), jnp.float32, low / len(cuts), high / len(cuts))
        level = level * jnp.repeat(jnp.exp(steps), dims[dim] // shards_of).reshape((-1,) + (1,) * (len(dims) - 1 - dim))
    return level


def scatter_about(stream_key, shape, width, reach, shards=(), held_as=jnp.bfloat16):
    drawn = jax.random.normal(stream_key, shape, jnp.float32) * width
    if len(shards) > 0:
        drawn = level_of(stream_key, shape, shards, -0.22, 0.18) * drawn
    return jnp.clip(drawn, min=-reach, max=reach).astype(held_as)


def setup_inputs(seed: int = 0) -> dict:
    key_list = jax.random.split(jax.random.key(seed), 20)
    tokens = scatter_about(key_list[0], (SEQ, D), 1.0, 6.0, ((0, 8), (1, 4)))
    pre_gain = jnp.clip(1.0 + 0.18 * jax.random.normal(key_list[1], (D,), jnp.float32), 0.1, 1.9)
    rate_factor = draw_rate_factor(jax.random.fold_in(key_list[19], 71), 0)
    w_rec_in = scatter_about(key_list[3], (D, LRU_W), D ** -0.5, 0.09375, ((1, 4),))
    w_rec_gate = draw_w_rec_gate(jax.random.fold_in(key_list[19], 71), 0)
    conv_taps = scatter_about(key_list[5], (CONV, LRU_W), 0.5, 3.0, ((1, 4),), jnp.float32)
    rate_maps = scatter_about(key_list[6], (LRU_W // LRU_BLK, LRU_BLK, LRU_BLK), LRU_BLK ** -0.5, 0.5, ((0, 4),))
    input_maps = scatter_about(key_list[7], (LRU_W // LRU_BLK, LRU_BLK, LRU_BLK), LRU_BLK ** -0.5, 0.5, ((0, 4),))
    decay_param = draw_decay_param(jax.random.fold_in(key_list[19], 71), 0)
    w_query = scatter_about(key_list[9], (D, HEADS * (NOPE + ROPE)), D ** -0.5, 0.09375, ((1, 4),))
    w_latent = scatter_about(key_list[10], (D, LATENT), D ** -0.5, 0.09375)
    w_rope_key = scatter_about(key_list[11], (D, ROPE), D ** -0.5, 0.09375)
    latent_gain = draw_latent_gain(jax.random.fold_in(key_list[19], 71), 0)
    w_expand = draw_w_expand(jax.random.fold_in(key_list[19], 71), 0)
    rec_gain = jnp.clip(1.0 + 0.18 * jax.random.normal(key_list[14], (LRU_W,), jnp.float32), 0.1, 1.9)
    att_gain = jnp.clip(1.0 + 0.18 * jax.random.normal(key_list[15], (HEADS * VDIM,), jnp.float32), 0.1, 1.9)
    w_out_rec = scatter_about(key_list[16], (LRU_W, D), (LRU_W + HEADS * VDIM) ** -0.5, 0.125, ((0, 4),))
    w_out_att = scatter_about(key_list[17], (HEADS * VDIM, D), (LRU_W + HEADS * VDIM) ** -0.5, 0.125, ((0, 4),))
    post_gain = jnp.clip(1.0 + 0.18 * jax.random.normal(key_list[18], (D,), jnp.float32), 0.1, 1.9)
    return {"tokens": tokens, "pre_gain": pre_gain, "rate_factor": rate_factor, "w_rec_in": w_rec_in, "w_rec_gate": w_rec_gate, "conv_taps": conv_taps, "rate_maps": rate_maps, "input_maps": input_maps, "decay_param": decay_param, "w_query": w_query, "w_latent": w_latent, "w_rope_key": w_rope_key, "latent_gain": latent_gain, "w_expand": w_expand, "rec_gain": rec_gain, "att_gain": att_gain, "w_out_rec": w_out_rec, "w_out_att": w_out_att, "post_gain": post_gain}


EPS = 1e-06
RATE_C = 8.0
THETA = 10000.0

def rms_inverse(values):
    return lax.rsqrt(lax.optimization_barrier(jnp.mean(values * values, axis=-1, keepdims=True)) + EPS)

def rotate(values, cosine, sine_part):
    half_width = values.shape[-1] // 2
    leading = values[..., :half_width]
    trailing = values[..., half_width:]
    return jnp.concatenate([leading * cosine - trailing * sine_part, trailing * cosine + leading * sine_part], axis=-1)

def angles(length, offset, span_width):
    frequency = 1.0 / THETA ** (jnp.arange(0, span_width, 2).astype(jnp.float32) / span_width)
    places = (offset + jnp.arange(length).astype(jnp.int32)).astype(jnp.float32)
    turned = places[:, None] * frequency[None, :]
    return (jnp.cos(turned), jnp.sin(turned))

def combine_steps(earlier, later):
    return (earlier[0] * later[0], later[0] * earlier[1] + later[1])

def attend_block(state_now, query_nope, query_rope, places, keys_nope, key_rope, values, key_root):
    maxima, totals, accumulated = state_now
    scaling = 1.0 / math.sqrt(query_nope.shape[-1] + query_rope.shape[-1])
    scores = jnp.einsum('qhd,khd->hqk', query_nope.astype(jnp.float32), keys_nope.astype(jnp.float32))
    scores = scores + jnp.einsum('qhd,kd->hqk', query_rope.astype(jnp.float32), key_rope.astype(jnp.float32))
    scores = scores * scaling
    key_places = key_root + jnp.arange(keys_nope.shape[0]).astype(jnp.int32)
    visible = key_places[None, :] <= places[:, None]
    scores = jnp.where(visible[None], scores, -jnp.inf)
    largest = jnp.maximum(maxima, lax.optimization_barrier(jnp.max(scores, axis=-1)))
    anchor = jnp.where(largest == -jnp.inf, 0.0, largest)
    weights = jnp.exp(scores - anchor[..., None])
    shrink = jnp.exp(maxima - anchor)
    totals = totals * shrink + lax.optimization_barrier(jnp.sum(weights, axis=-1))
    rounded = weights.astype(jnp.bfloat16).astype(jnp.float32)
    accumulated = accumulated * shrink[..., None] + jnp.einsum('hqk,khd->hqd', rounded, values.astype(jnp.float32))
    return (largest, totals, accumulated)

def reference(tokens, pre_gain, rate_factor, w_rec_in, w_rec_gate, conv_taps, rate_maps, input_maps, decay_param, w_query, w_latent, w_rope_key, latent_gain, w_expand, rec_gain, att_gain, w_out_rec, w_out_att, post_gain):
    tokens_wide = tokens.astype(jnp.float32)
    inverse = rms_inverse(tokens_wide)
    scaled = (tokens_wide * pre_gain).astype(jnp.bfloat16)

    def project(weight):
        return inverse * jnp.dot(scaled, weight, preferred_element_type=jnp.float32)
    rec_input = project(w_rec_in).astype(jnp.bfloat16)
    gate_value = project(w_rec_gate)
    query_raw = project(w_query)
    latent_raw = project(w_latent)
    rope_raw = project(w_rope_key)
    padded = jnp.concatenate([jnp.zeros((CONV - 1, LRU_W), jnp.bfloat16), rec_input], axis=0)
    convolved = conv_taps[0] * padded[0:SEQ].astype(jnp.float32)
    for tap_index in range(1, CONV):
        convolved = convolved + conv_taps[tap_index] * padded[tap_index:tap_index + SEQ].astype(jnp.float32)
    conv_low = lax.optimization_barrier(convolved.astype(jnp.bfloat16)).astype(jnp.float32)
    blocks = conv_low.reshape(SEQ, LRU_W // LRU_BLK, LRU_BLK)
    rate_gate = jax.nn.sigmoid(jnp.einsum('sbi,bij->sbj', blocks, rate_maps.astype(jnp.float32))).reshape(SEQ, LRU_W)
    entry_gate = jax.nn.sigmoid(jnp.einsum('sbi,bij->sbj', blocks, input_maps.astype(jnp.float32))).reshape(SEQ, LRU_W)
    log_keep = -RATE_C * rate_factor[:, None] * rate_gate * jax.nn.softplus(-decay_param)
    keep_rate = jnp.exp(log_keep)
    driven = jnp.sqrt(-jnp.expm1(2.0 * log_keep)) * entry_gate * convolved
    state_seq = lax.associative_scan(combine_steps, (keep_rate, driven), axis=0)[1]
    rec_out = state_seq * jax.nn.gelu(gate_value)
    rec_norm = (rec_out * rms_inverse(rec_out) * rec_gain).astype(jnp.bfloat16)
    cosine, sine_part = angles(SEQ, 0, ROPE)
    query_heads = query_raw.reshape(SEQ, HEADS, NOPE + ROPE)
    query_nope = query_heads[:, :, :NOPE].astype(jnp.bfloat16)
    query_rope = rotate(query_heads[:, :, NOPE:], cosine[:, None, :], sine_part[:, None, :]).astype(jnp.bfloat16)
    latent_norm = (latent_raw * rms_inverse(latent_raw) * latent_gain).astype(jnp.bfloat16)
    rope_key = rotate(rope_raw, cosine, sine_part).astype(jnp.bfloat16)
    expanded = jnp.dot(latent_norm, w_expand, preferred_element_type=jnp.float32).astype(jnp.bfloat16)
    expanded = expanded.reshape(SEQ, HEADS, NOPE + VDIM)
    keys_nope = expanded[:, :, :NOPE]
    values = expanded[:, :, NOPE:]
    query_span = math.gcd(SEQ, 256)
    block_count = SEQ // query_span

    def one_block(block_index):
        root = block_index * query_span
        block_nope = lax.dynamic_slice_in_dim(query_nope, root, query_span, 0)
        block_rope = lax.dynamic_slice_in_dim(query_rope, root, query_span, 0)
        places = root + jnp.arange(query_span).astype(jnp.int32)
        initial = (jnp.full((HEADS, query_span), -jnp.inf, jnp.float32), jnp.zeros((HEADS, query_span), jnp.float32), jnp.zeros((HEADS, query_span, VDIM), jnp.float32))
        maxima, totals, accumulated = attend_block(initial, block_nope, block_rope, places, keys_nope, rope_key, values, 0)
        return (accumulated / totals[..., None]).transpose(1, 0, 2)
    att_out = lax.map(one_block, jnp.arange(block_count).astype(jnp.int32)).reshape(SEQ, HEADS * VDIM)
    att_norm = (att_out * rms_inverse(att_out) * att_gain).astype(jnp.bfloat16)
    rec_width = LRU_W // N_TP
    att_width = HEADS * VDIM // N_TP
    mixed_sum = jnp.zeros((SEQ, D), jnp.float32)
    for member in range(N_TP):
        partial_value = jnp.dot(rec_norm[:, member * rec_width:(member + 1) * rec_width], w_out_rec[member * rec_width:(member + 1) * rec_width], preferred_element_type=jnp.float32)
        partial_value = partial_value + jnp.dot(att_norm[:, member * att_width:(member + 1) * att_width], w_out_att[member * att_width:(member + 1) * att_width], preferred_element_type=jnp.float32)
        mixed_sum = mixed_sum + lax.optimization_barrier(partial_value.astype(jnp.bfloat16)).astype(jnp.float32)
    return (mixed_sum * rms_inverse(mixed_sum) * post_gain).astype(jnp.bfloat16)
```

```python
import functools
import math

import jax
import jax.numpy as jnp
from jax import lax
from jax.experimental import pallas as pl
from jax.experimental.pallas import tpu as pltpu
from jax.sharding import PartitionSpec as P

NOPE = 128
ROPE = 64
VDIM = 128
EPS = 1e-06
RATE_C = 8.0
THETA = 10000.0
F32 = jnp.float32
BF16 = jnp.bfloat16


VMEM = pl.BlockSpec(memory_space=pltpu.VMEM)
SMEM = pl.BlockSpec(memory_space=pltpu.SMEM)


def params(mib):
    return pltpu.CompilerParams(vmem_limit_bytes=mib << 20)


def cost(flops, moved=0):
    return pl.CostEstimate(flops=flops, bytes_accessed=moved, transcendentals=0)


def swap(block, axis, mask):
    return lax.ppermute(block, axis, [(i, i ^ mask) for i in range(lax.axis_size(axis))])


def dot(a, b):
    return jnp.dot(a, b, preferred_element_type=F32)


def dot_t(a, b):
    return lax.dot_general(a, b, (((1,), (1,)), ((), ())), preferred_element_type=F32)


def as_row(column):
    return jnp.transpose(jnp.broadcast_to(column, (column.shape[0], 128)))[:8]


def as_column(row):
    return jnp.transpose(jnp.broadcast_to(row, (128, row.shape[1])))[:, :1]


def turned(values, cosine, sine):
    half = values.shape[1] // 2
    u, w = values[:, :half], values[:, half:]
    return jnp.concatenate([u * cosine - w * sine, w * cosine + u * sine], axis=1)


def project_body(count, first, last, ids, *refs):
    pieces, refs = refs[:count], refs[count:]
    gain, refs = refs[0], refs[1:]
    weights, refs = refs[:5], refs[5:]
    if not first:
        before, refs = refs[:6], refs[6:]
    if last:
        (cosine, sine, latent_gain), refs = refs[:3], refs[3:]
    sums = [None] * 5
    squares = None
    for n in range(count):
        wide = pieces[n][...].astype(F32)
        part = jnp.sum(wide * wide, axis=1, keepdims=True)
        squares = part if squares is None else squares + part
        low = (wide * gain[ids[n]]).astype(BF16)
        for k in range(5):
            product = dot(low, weights[k][ids[n]])
            sums[k] = product if sums[k] is None else sums[k] + product
    if not first:
        sums = [s + b[...] for s, b in zip(sums, before)]
        squares = squares + before[5][...]
    if not last:
        for out, s in zip(refs, sums):
            out[...] = s
        refs[5][...] = squares
        return
    rec_input, gate, query, latent = refs
    width = gain.shape[0] * gain.shape[2]
    inverse = lax.rsqrt(squares / width + EPS)
    rec_input[...] = (inverse * sums[0]).astype(BF16)
    gate[...] = inverse * sums[1]
    raw = inverse * sums[2]
    c, s = cosine[...], sine[...]
    for h in range(query.shape[0]):
        base = h * (NOPE + ROPE)
        query[h, :, :NOPE] = raw[:, base : base + NOPE].astype(BF16)
        query[h, :, NOPE:] = turned(raw[:, base + NOPE : base + NOPE + ROPE], c, s).astype(BF16)
    raw = inverse * sums[3]
    norm = lax.rsqrt(jnp.mean(raw * raw, axis=1, keepdims=True) + EPS)
    span = raw.shape[1]
    latent[:, :span] = (raw * norm * latent_gain[...]).astype(BF16)
    latent[:, span:] = turned(inverse * sums[4], c, s).astype(BF16)


def shifted(values, distance, fill):
    rows = lax.broadcasted_iota(jnp.int32, values.shape, 0)
    return jnp.where(rows >= distance, pltpu.roll(values, distance, 0), fill)


def recur_body(rec_input, tail, taps, rate_maps, input_maps, decay, factor, local, cum, ends):
    rows, channels = rec_input.shape
    own = rec_input[...].astype(F32)
    before = tail[...].astype(F32)
    count = taps.shape[0]
    index = lax.broadcasted_iota(jnp.int32, own.shape, 0)
    padded = jnp.concatenate([before, jnp.zeros((rows - 8, channels), F32)], axis=0)
    convolved = None
    for k in range(count):
        back = count - 1 - k
        if back:
            here = jnp.where(index >= back, pltpu.roll(own, back, 0), pltpu.roll(padded, rows - 8 + back, 0))
        else:
            here = own
        term = taps[k : k + 1, :] * here
        convolved = term if convolved is None else convolved + term
    low = convolved.astype(BF16)
    width = rate_maps.shape[1]
    rates, entries = [], []
    for b in range(rate_maps.shape[0]):
        part = low[:, b * width : (b + 1) * width]
        rates.append(dot(part, rate_maps[b]))
        entries.append(dot(part, input_maps[b]))
    rate_gate = jax.nn.sigmoid(jnp.concatenate(rates, axis=1))
    entry_gate = jax.nn.sigmoid(jnp.concatenate(entries, axis=1))
    log_keep = -RATE_C * factor[...] * rate_gate * decay[...]
    keep = jnp.exp(log_keep)
    y = -2.0 * log_keep
    series = 1.0 - y / 6.0
    for n in (5.0, 4.0, 3.0, 2.0):
        series = 1.0 - y / n * series
    lost = jnp.where(y < 0.125, y * series, 1.0 - jnp.exp(-y))
    state = jnp.sqrt(lost) * entry_gate * convolved
    distance = 1
    while distance < rows:
        state = keep * shifted(state, distance, 0.0) + state
        keep = keep * shifted(keep, distance, 1.0)
        distance *= 2
    local[...] = state
    cum[...] = keep
    ends[0:1, :] = keep[rows - 1 :]
    ends[1:8, :] = jnp.broadcast_to(state[rows - 1 :], (7, channels))


def finish_recur_body(local, cum, carried, gate, out, stats):
    state = local[...] + cum[...] * carried[1:2, :]
    value = state * jax.nn.gelu(gate[...])
    out[...] = value
    stats[...] = as_row(jnp.sum(value * value, axis=1, keepdims=True))


def attend_body(pairs, me, query, own, *refs):
    halves, refs = refs[: 2 * (pairs - 1)], refs[2 * (pairs - 1) :]
    expand, out, stats, held, scores, most, total, gathered = refs
    heads, rows, width = query.shape
    span = expand.shape[0]
    scaling = 1.0 / math.sqrt(width)
    mine = me[0]

    def expanded(n, parts):
        top = 0
        for part in parts:
            size = part.shape[0]
            held[n, top : top + size, :] = dot(part[:, :span], expand[...]).astype(BF16)
            top += size
        rope = [part[:, span:] for part in parts]
        rope = rope[0] if len(rope) == 1 else jnp.concatenate(rope, axis=0)
        for h in range(heads):
            base = h * (NOPE + VDIM)
            key = jnp.concatenate([held[n, :, base : base + NOPE], rope], axis=1)
            yield h, dot_t(query[h], key) * scaling

    def widest(values):
        found = values[:, :128]
        for n in range(128, values.shape[1], 128):
            found = jnp.maximum(found, values[:, n : n + 128])
        return found

    def summed(values):
        found = values[:, :128]
        for n in range(128, values.shape[1], 128):
            found = found + values[:, n : n + 128]
        return found

    place = lax.broadcasted_iota(jnp.int32, (rows, rows), 0)
    key_place = lax.broadcasted_iota(jnp.int32, (rows, rows), 1)
    for h, value in expanded(0, [own[...]]):
        value = jnp.where(key_place <= place, value, -jnp.inf)
        scores[h, 0] = value
        most[h] = widest(value)
    for n in range(1, pairs):

        @pl.when((mine ^ n) < mine)
        def _(n=n):
            for h, value in expanded(n, [halves[2 * n - 2][...], halves[2 * n - 1][...]]):
                scores[h, n] = value
                most[h] = jnp.maximum(most[h], widest(value))

    for h in range(heads):
        base = h * (NOPE + VDIM) + NOPE
        most[h] = jnp.broadcast_to(jnp.max(most[h], axis=1, keepdims=True), (rows, 128))

        def weigh(n, h=h, base=base):
            weights = jnp.exp(scores[h, n] - most[h][:, :1])
            return summed(weights), dot(weights.astype(BF16), held[n, :, base : base + VDIM])

        total[h], gathered[h] = weigh(0)
        for n in range(1, pairs):

            @pl.when((mine ^ n) < mine)
            def _(n=n, h=h, weigh=weigh):
                more, values = weigh(n)
                total[h] = total[h] + more
                gathered[h] = gathered[h] + values

    squares = None
    for h in range(heads):
        value = gathered[h] / jnp.sum(total[h], axis=1, keepdims=True)
        out[:, h * VDIM : (h + 1) * VDIM] = value
        part = jnp.sum(value * value, axis=1, keepdims=True)
        squares = part if squares is None else squares + part
    stats[...] = as_row(squares)


def merge_body(widths, ids, rec, att, rec_total, att_total, rec_gain, att_gain, w_rec, w_att, out, norms):
    blocks, size, _ = out.shape
    channels = rec.shape[1]
    rec_scale = as_column(lax.rsqrt(rec_total[0:1, :] / widths[0] + EPS))
    att_scale = as_column(lax.rsqrt(att_total[0:1, :] / widths[1] + EPS))
    norms[:, :channels] = rec[...] * rec_scale * rec_gain[...]
    norms[:, channels:] = att[...] * att_scale * att_gain[...]
    picked = [norms[pl.ds(pl.multiple_of(ids[b] * size, 8), size), :] for b in range(blocks)]
    picked = jnp.concatenate(picked, axis=0).astype(BF16)
    step = 1024
    for n in range(0, w_rec.shape[1], step):
        value = dot(picked[:, :channels], w_rec[:, n : n + step])
        value = value + dot(picked[:, channels:], w_att[:, n : n + step])
        value = value.astype(BF16)
        for b in range(blocks):
            out[b, :, n : n + step] = value[b * size : (b + 1) * size]


def close_body(count, gain, keep, arrived, *refs):
    parts, out = refs[:count], refs[count]
    mixed = keep[0].astype(F32) + arrived[0].astype(F32)
    for part in parts:
        mixed = mixed + part[...].astype(F32)
    scale = lax.rsqrt(jnp.mean(mixed * mixed, axis=1, keepdims=True) + EPS)
    out[...] = (mixed * scale * gain[...]).astype(BF16)


def shards(
    tokens,
    pre_gain,
    rate_factor,
    w_rec_in,
    w_rec_gate,
    conv_taps,
    rate_maps,
    input_maps,
    decay_param,
    w_query,
    w_latent,
    w_rope_key,
    latent_gain,
    w_expand,
    rec_gain,
    att_gain,
    w_out_rec,
    w_out_att,
    post_gain,
):
    rows, depth = tokens.shape
    model_width, channels = w_rec_in.shape
    heads = w_query.shape[1] // (NOPE + ROPE)
    span = w_latent.shape[1]
    group = lax.axis_size("tp")
    chain = lax.axis_size("sp")
    lane = lax.axis_index("tp")
    place = lax.axis_index("sp")
    shape = jax.ShapeDtypeStruct

    pieces = {0: tokens, 1: swap(tokens, "tp", 1)}
    half = rows // 2
    for m in range(2, group, 2):
        top = swap(tokens[:half], "tp", m)
        low = swap(tokens[half:], "tp", m)
        top_more, low_more = swap(top, "tp", 1), swap(low, "tp", 1)
        pieces[m] = jnp.concatenate([top, low], axis=0)
        pieces[m + 1] = jnp.concatenate([top_more, low_more], axis=0)

    frequency = 1.0 / THETA ** (jnp.arange(0, ROPE, 2).astype(F32) / ROPE)
    places = (place * rows + jnp.arange(rows)).astype(F32)
    angle = places[:, None] * frequency[None, :]
    cosine, sine = jnp.cos(angle), jnp.sin(angle)
    decay = jax.nn.softplus(-decay_param)[None, :]
    factor = rate_factor[:, None]

    weights = [
        w.reshape(group, depth, w.shape[1])
        for w in (w_rec_in, w_rec_gate, w_query, w_latent, w_rope_key)
    ]
    gain = pre_gain.reshape(group, 1, depth)
    widths = [w.shape[2] for w in weights]
    flops = 2 * rows * depth * sum(widths)
    order = lane ^ jnp.arange(group, dtype=jnp.int32)
    sums = pl.pallas_call(
        functools.partial(project_body, 2, True, False),
        out_shape=[shape((rows, w), F32) for w in widths] + [shape((rows, 1), F32)],
        in_specs=[SMEM] + [VMEM] * 8,
        out_specs=[VMEM] * 6,
        compiler_params=params(16),
        cost_estimate=cost(2 * flops),
        name="project_first",
    )(order[:2], pieces[0], pieces[1], gain, *weights)
    rest = [pieces[m] for m in range(2, group)]
    rec_input, gate_value, query, latent = pl.pallas_call(
        functools.partial(project_body, group - 2, False, True),
        out_shape=[
            shape((rows, channels), BF16),
            shape((rows, channels), F32),
            shape((heads, rows, NOPE + ROPE), BF16),
            shape((rows, span + ROPE), BF16),
        ],
        in_specs=[SMEM] + [VMEM] * (group - 2 + 6 + 6 + 3),
        out_specs=[VMEM] * 4,
        compiler_params=params(16),
        cost_estimate=cost((group - 2) * flops),
        name="project_rest",
    )(order[2:], *rest, gain, *weights, *sums, cosine, sine, latent_gain[None, :])

    low_core = lane % 2 == 0
    mine = jnp.where(low_core, latent[:half], latent[half:])
    reached = {}
    for m in range(2, chain, 2):
        reached[m] = swap(mine, "sp", m)
    reached[1] = swap(mine, "sp", 1)
    for m in range(2, chain, 2):
        reached[m + 1] = swap(reached[m], "sp", 1)
    others = {m: swap(reached[m], "tp", 1) for m in reached}

    devices = range(chain)
    tail = lax.ppermute(rec_input[rows - 8 :], "sp", [(i, i + 1) for i in devices if i + 1 < chain])
    local, cum, ends = pl.pallas_call(
        recur_body,
        out_shape=[
            shape((rows, channels), F32),
            shape((rows, channels), F32),
            shape((8, channels), F32),
        ],
        in_specs=[VMEM] * 7,
        out_specs=[VMEM] * 3,
        compiler_params=params(16),
        cost_estimate=cost(2 * rows * channels * 2000),
        name="recur",
    )(rec_input, tail, conv_taps, rate_maps, input_maps, decay, factor)
    reach = 1
    whole = ends
    prefix = jnp.concatenate([jnp.ones((1, channels), F32), jnp.zeros((7, channels), F32)], axis=0)
    first_row = lax.broadcasted_iota(jnp.int32, ends.shape, 0) == 0

    def combined(earlier, later):
        return jnp.where(first_row, earlier * later, later[0:1] * earlier + later)

    while reach < chain:
        theirs = swap(whole, "sp", reach)
        behind = (place & reach) != 0
        prefix = jnp.where(behind, combined(theirs, prefix), prefix)
        whole = jnp.where(behind, combined(theirs, whole), combined(whole, theirs))
        reach *= 2
    rec_out, rec_squares = pl.pallas_call(
        finish_recur_body,
        out_shape=[shape((rows, channels), F32), shape((8, rows), F32)],
        in_specs=[VMEM] * 4,
        out_specs=[VMEM] * 2,
        compiler_params=params(16),
        cost_estimate=cost(2 * rows * channels * 500),
        name="finish_recur",
    )(local, cum, prefix, gate_value)
    rec_total = lax.psum(rec_squares, "tp")

    keys = []
    for m in range(1, chain):
        keys += [reached[m], others[m]]
    att_out, att_squares = pl.pallas_call(
        functools.partial(attend_body, chain),
        out_shape=[shape((rows, heads * VDIM), F32), shape((8, rows), F32)],
        in_specs=[SMEM] + [VMEM] * (len(keys) + 3),
        out_specs=[VMEM] * 2,
        scratch_shapes=[
            pltpu.VMEM((chain, rows, w_expand.shape[1]), BF16),
            pltpu.VMEM((heads, chain, rows, rows), F32),
            pltpu.VMEM((heads, rows, 128), F32),
            pltpu.VMEM((heads, rows, 128), F32),
            pltpu.VMEM((heads, rows, VDIM), F32),
        ],
        compiler_params=params(32),
        cost_estimate=cost(8 * rows * rows * chain * 1000),
        name="attend",
    )(place[None], query, latent, *keys, w_expand)
    att_total = lax.psum(att_squares, "tp")

    size = rows // group
    even = jnp.arange(0, group, 2, dtype=jnp.int32)
    merge = pl.pallas_call(
        functools.partial(merge_body, (channels * group, heads * VDIM * group)),
        out_shape=shape((group // 2, size, model_width), BF16),
        in_specs=[SMEM] + [VMEM] * 8,
        out_specs=VMEM,
        scratch_shapes=[pltpu.VMEM((rows, channels + heads * VDIM), F32)],
        compiler_params=params(16),
        cost_estimate=cost(2 * rows * (channels + heads * VDIM) * model_width // 2),
        name="merge",
    )
    operands = (
        rec_out, att_out, rec_total, att_total, rec_gain[None, :], att_gain[None, :], w_out_rec, w_out_att
    )
    sent = merge((lane ^ 1) ^ even, *operands)
    arrived = swap(sent, "tp", 1)
    kept = merge(lane ^ even, *operands)
    parts = []
    for n in range(1, group // 2):
        chip = (kept[n].astype(F32) + arrived[n].astype(F32)).astype(BF16)
        parts.append(swap(chip, "tp", 2 * n))
    return pl.pallas_call(
        functools.partial(close_body, len(parts)),
        out_shape=shape((size, model_width), BF16),
        in_specs=[VMEM] * (3 + len(parts)),
        out_specs=VMEM,
        compiler_params=params(16),
        cost_estimate=cost(size * model_width * 100),
        name="close",
    )(post_gain[None, :], kept[:1], arrived[:1], *parts)


def solution(mesh):
    placed = (
        P("sp", "tp"),
        P(),
        P("sp"),
        P(None, "tp"),
        P(None, "tp"),
        P(None, "tp"),
        P("tp", None, None),
        P("tp", None, None),
        P("tp"),
        P(None, "tp"),
        P(),
        P(),
        P(),
        P(None, "tp"),
        P("tp"),
        P("tp"),
        P("tp", None),
        P("tp", None),
        P(),
    )
    return jax.shard_map(
        shards, mesh=mesh, in_specs=placed, out_specs=P(("sp", "tp"), None), check_vma=False
    )
```

```python
import functools
import math

import jax
import jax.numpy as jnp
from jax import lax
from jax.experimental import pallas as pl
from jax.experimental.pallas import tpu as pltpu
from jax.sharding import PartitionSpec as P


NOPE = 128
ROPE = 64
VDIM = 128
EPS = 1e-06
RATE_C = 8.0
THETA = 10000.0
F32 = jnp.float32
BF16 = jnp.bfloat16


VMEM = pl.BlockSpec(memory_space=pltpu.VMEM)
HBM = pl.BlockSpec(memory_space=pltpu.HBM)


def params(mib):
    return pltpu.CompilerParams(vmem_limit_bytes=mib << 20)


def cost(flops, moved=0):
    return pl.CostEstimate(flops=flops, bytes_accessed=moved, transcendentals=0)


def swap(block, axis, mask):
    return lax.ppermute(block, axis, [(i, i ^ mask) for i in range(lax.axis_size(axis))])


def kernel(body, **settings):
    return pl.pallas_call(body, **settings)


def in_hbm(array):
    return pltpu.with_memory_space_constraint(array, pltpu.HBM)


def dot(a, b):
    return jnp.dot(a, b, preferred_element_type=F32)


def dot_t(a, b):
    return lax.dot_general(a, b, (((1,), (1,)), ((), ())), preferred_element_type=F32)


def as_row(column):
    return jnp.transpose(jnp.broadcast_to(column, (column.shape[0], 128)))[:8]


def as_column(row):
    return jnp.transpose(jnp.broadcast_to(row, (128, row.shape[1])))[:, :1]


def turned(values, cosine, sine):
    half = values.shape[1] // 2
    u, w = values[:, :half], values[:, half:]
    return jnp.concatenate([u * cosine - w * sine, w * cosine + u * sine], axis=1)


def split_body(tokens, *refs):
    outs, ending, sems = refs[:-2], refs[-2], refs[-1]
    rows = tokens.shape[0]
    copies = [pltpu.make_async_copy(tokens.at[rows - 8 :, :], ending, sems.at[len(outs)])]
    copies[0].start()
    base = 0
    for n, out in enumerate(outs):
        width = out.shape[1]
        copies.append(pltpu.make_async_copy(tokens.at[:, base : base + width], out, sems.at[n]))
        copies[n + 1].start()
        base += width
    for copy in copies:
        copy.wait()


def project_body(places, ahead, last, *refs):
    count = len(places)
    blocks, refs = refs[:count], refs[count:]
    halos, refs = refs[:count], refs[count:]
    (gain, *weights), refs = refs[:6], refs[6:]
    if ahead is None:
        before, refs = refs[:8], refs[8:]
    if last:
        (cosine, sine, latent_gain), refs = refs[:3], refs[3:]
    lane = lax.axis_index("tp")
    depth = gain.shape[2]
    size = blocks[0].shape[1]
    copies = {}
    if ahead is None:
        held = weights
    else:
        held, sems, refs = refs[-6:-1], refs[-1], refs[:-6]
        targets = [(held, places, size)]
        used = 8
        for some, width in ahead:
            targets.append((refs[used : used + 5], some, width))
            used += 5
        for t, (buffers, some, width) in enumerate(targets):
            for n, (piece, column) in enumerate(some):
                start = pl.multiple_of((lane ^ piece) * depth + column, 128)
                for k in range(5):
                    span = pl.ds(start, width)
                    source = weights[k].at[:, span] if k == 4 else weights[k].at[span, :]
                    copy = pltpu.make_async_copy(source, buffers[k].at[n], sems.at[t, n, k])
                    copy.start()
                    copies[t, n, k] = copy
    sums = [None] * 5
    squares, halo_sum, halo_squares = None, None, None

    def plus(total, part):
        return part if total is None else total + part

    for n, (piece, column) in enumerate(places):
        scale = gain[lane ^ piece][:, column : column + size]
        wide = blocks[n][...].astype(F32)
        squares = plus(squares, jnp.sum(wide * wide, axis=1, keepdims=True))
        low = (wide * scale).astype(BF16)
        edge = halos[n][...].astype(F32)[:, column : column + size]
        halo_squares = plus(halo_squares, jnp.sum(edge * edge, axis=1, keepdims=True))
        edge = (edge * scale).astype(BF16)
        for k in range(5):
            if copies:
                copies[0, n, k].wait()
            sums[k] = plus(sums[k], dot_t(low, held[k][n]) if k == 4 else dot(low, held[k][n]))
            if k == 0:
                halo_sum = plus(halo_sum, dot(edge, held[k][n]))
    parts = sums + [squares, halo_sum, halo_squares]
    if ahead is None:
        parts = [part + b[...] for part, b in zip(parts, before)]
    if not last:
        for out, part in zip(refs, parts):
            out[...] = part
        for key, copy in copies.items():
            if key[0]:
                copy.wait()
        return
    sums, (squares, halo_sum, halo_squares) = parts[:5], parts[5:]
    rec_input, tail, gate, query, latent, mine = refs
    width = gain.shape[0] * depth
    inverse = lax.rsqrt(squares / width + EPS)
    c, s = cosine[...], sine[...]
    raw = inverse * sums[3]
    norm = lax.rsqrt(jnp.mean(raw * raw, axis=1, keepdims=True) + EPS)
    span = raw.shape[1]
    latent[:, :span] = (raw * norm * latent_gain[...]).astype(BF16)
    latent[:, span:] = turned(inverse * sums[4], c, s).astype(BF16)
    half = mine.shape[0]
    mine[...] = latent[pl.ds(pl.multiple_of((lane & 1) * half, half), half), :]
    rec_input[...] = (inverse * sums[0]).astype(BF16)
    tail[...] = (lax.rsqrt(halo_squares / width + EPS) * halo_sum).astype(BF16)
    gate[...] = inverse * sums[1]
    raw = inverse * sums[2]
    for h in range(query.shape[0]):
        base = h * (NOPE + ROPE)
        query[h, :, :NOPE] = raw[:, base : base + NOPE].astype(BF16)
        query[h, :, NOPE:] = turned(raw[:, base + NOPE : base + NOPE + ROPE], c, s).astype(BF16)


def shifted(values, distance, fill):
    rows = lax.broadcasted_iota(jnp.int32, values.shape, 0)
    return jnp.where(rows >= distance, pltpu.roll(values, distance, 0), fill)


def recur_body(rec_input, tail, taps, rate_maps, input_maps, decay, factor, local, cum, ends):
    rows, channels = rec_input.shape
    own = rec_input[...].astype(F32)
    before = tail[...].astype(F32)
    count = taps.shape[0]
    index = lax.broadcasted_iota(jnp.int32, own.shape, 0)
    padded = jnp.concatenate([before, jnp.zeros((rows - 8, channels), F32)], axis=0)
    convolved = None
    for k in range(count):
        back = count - 1 - k
        if back:
            here = jnp.where(index >= back, pltpu.roll(own, back, 0), pltpu.roll(padded, rows - 8 + back, 0))
        else:
            here = own
        term = taps[k : k + 1, :] * here
        convolved = term if convolved is None else convolved + term
    low = convolved.astype(BF16)
    width = rate_maps.shape[1]
    rates, entries = [], []
    for b in range(rate_maps.shape[0]):
        part = low[:, b * width : (b + 1) * width]
        rates.append(dot(part, rate_maps[b]))
        entries.append(dot(part, input_maps[b]))
    rate_gate = jax.nn.sigmoid(jnp.concatenate(rates, axis=1))
    entry_gate = jax.nn.sigmoid(jnp.concatenate(entries, axis=1))
    log_keep = -RATE_C * as_column(factor[...]) * rate_gate * decay[...]
    keep = jnp.exp(log_keep)
    y = -2.0 * log_keep
    series = 1.0 - y / 6.0
    for n in (5.0, 4.0, 3.0, 2.0):
        series = 1.0 - y / n * series
    lost = jnp.where(y < 0.125, y * series, 1.0 - jnp.exp(-y))
    state = jnp.sqrt(lost) * entry_gate * convolved
    distance = 1
    while distance < rows:
        state = keep * shifted(state, distance, 0.0) + state
        keep = keep * shifted(keep, distance, 1.0)
        distance *= 2
    local[...] = state
    cum[...] = keep
    ends[0:1, :] = keep[rows - 1 :]
    ends[1:8, :] = jnp.broadcast_to(state[rows - 1 :], (7, channels))


def combined(earlier, later):
    first_row = lax.broadcasted_iota(jnp.int32, earlier.shape, 0) == 0
    return jnp.where(first_row, earlier * later, later[0:1] * earlier + later)


def behind(reach):
    return (lax.axis_index("sp") & reach) != 0


def taken(reach, theirs, prefix):
    if prefix is None:
        neutral = lax.broadcasted_iota(jnp.int32, theirs.shape, 0) == 0
        return jnp.where(behind(reach), theirs, jnp.where(neutral, 1.0, 0.0))
    return jnp.where(behind(reach), combined(theirs, prefix), prefix)


def pass_on_body(reach, whole, theirs, *refs):
    prefix, (whole_out, prefix_out) = refs[:-2], refs[-2:]
    mine, other = whole[...], theirs[...]
    prefix_out[...] = taken(reach, other, prefix[0][...] if prefix else None)
    whole_out[...] = jnp.where(behind(reach), combined(other, mine), combined(mine, other))


def finish_recur_body(reach, local, cum, gate, theirs, *refs):
    prefix, (out, stats) = refs[:-2], refs[-2:]
    carried = taken(reach, theirs[...], prefix[0][...] if prefix else None)
    state = local[...] + cum[...] * carried[1:2, :]
    value = state * jax.nn.gelu(gate[...])
    out[...] = value
    stats[...] = as_row(jnp.sum(value * value, axis=1, keepdims=True))


def attend_body(masks, before_count, fetch, last, query, *refs):
    own = masks == [0]
    count = 1 if own else 2 * len(masks)
    keys, refs = refs[:count], refs[count:]
    expand, refs = refs[0], refs[1:]
    before, refs = refs[:before_count], refs[before_count:]
    copies = []
    if fetch:
        sources, refs, sems = refs[:2], refs[2:-1], refs[-1]
        for n, (source, target) in enumerate(zip(sources, refs[3:5])):
            copies.append(pltpu.make_async_copy(source, target, sems.at[n]))
            copies[n].start()
    if last:
        rec_stats, out, stats = refs
    else:
        most, total, gathered = refs[:3]
    heads, rows, width = query.shape
    span = expand.shape[0]
    scaling = 1.0 / math.sqrt(width)
    mine = lax.axis_index("sp")
    values = jnp.concatenate([key[...] for key in keys], axis=0)
    expanded = dot(values[:, :span], expand[...]).astype(BF16)
    rope = values[:, span:]
    if own:
        place = lax.broadcasted_iota(jnp.int32, (rows, rows), 0)
        hidden = lax.broadcasted_iota(jnp.int32, (rows, rows), 1) > place
    squares = None
    for h in range(heads):
        base = h * (NOPE + VDIM)
        key = jnp.concatenate([expanded[:, base : base + NOPE], rope], axis=1)
        scores = dot_t(query[h], key) * scaling
        if own:
            scores = jnp.where(hidden, -jnp.inf, scores)
        else:
            parts = []
            for n, mask in enumerate(masks):
                part = scores[:, n * rows : (n + 1) * rows]
                parts.append(part + jnp.where((mine ^ mask) < mine, 0.0, -jnp.inf))
            scores = jnp.concatenate(parts, axis=1)
        top = jnp.max(scores, axis=1, keepdims=True)
        if before:
            top = jnp.maximum(before[0][h][:, :1], top)
        weights = jnp.exp(scores - top)
        part = weights[:, :128]
        for n in range(128, scores.shape[1], 128):
            part = part + weights[:, n : n + 128]
        product = dot(weights.astype(BF16), expanded[:, base + NOPE : base + NOPE + VDIM])
        if before:
            shrink = jnp.exp(before[0][h][:, :1] - top)
            part = part + before[1][h] * shrink
            product = product + before[2][h] * shrink
        if not last:
            most[h] = jnp.broadcast_to(top, (rows, 128))
            total[h] = part
            gathered[h] = product
            continue
        value = product / jnp.sum(part, axis=1, keepdims=True)
        out[:, h * VDIM : (h + 1) * VDIM] = value
        part = jnp.sum(value * value, axis=1, keepdims=True)
        squares = part if squares is None else squares + part
    for copy in copies:
        copy.wait()
    if last:
        stats[:8] = rec_stats[...]
        stats[8:] = as_row(squares)


def merge_body(rec, att, rec_gain, att_gain, w_rec, w_att, rec_out, att_out, low_rec, low_att):
    lane = lax.axis_index("tp")
    group = lax.axis_size("tp")
    size = rec.shape[0] // group
    order = [1 ^ m for m in range(0, group, 2)] + list(range(0, group, 2))
    for n, mask in enumerate(order):
        rows = pl.ds(pl.multiple_of((lane ^ mask) * size, size), size)
        low_rec[n * size : (n + 1) * size] = (rec[rows, :] * rec_gain[...]).astype(BF16)
        low_att[n * size : (n + 1) * size] = (att[rows, :] * att_gain[...]).astype(BF16)
    step = 512
    for low, weight, out in ((low_rec, w_rec, rec_out), (low_att, w_att, att_out)):
        for n in range(0, out.shape[1], step):
            out[:, n : n + step] = dot(low[...], weight[:, n : n + step])


def scales(widths, totals):
    total = totals[0][...]
    for other in totals[1:]:
        total = total + other[...]
    scaled = []
    for k in range(2):
        scaled.append(as_column(lax.rsqrt(total[8 * k : 8 * k + 1, :] / widths[k] + EPS)))
    return scaled


def partial(widths, mask, position, columns, rec, att, totals, scratch):
    lane = lax.axis_index("tp")
    size = rec.shape[0] // lax.axis_size("tp")
    for k, scale in enumerate(scales(widths, totals)):
        scratch[k] = jnp.broadcast_to(scale, scratch.shape[1:])
    rows = pl.ds(pl.multiple_of((lane ^ mask) * size, size), size)
    here = slice(position * size, (position + 1) * size)
    value = scratch[0, rows, :][:, :1] * rec[here, columns]
    value = value + scratch[1, rows, :][:, :1] * att[here, columns]
    return value.astype(BF16)


def send_body(widths, mask, position, columns, rec, att, *refs):
    totals, (out, scratch) = refs[:-2], refs[-2:]
    out[...] = partial(widths, mask, position, columns, rec, att, totals, scratch)


def chip_body(widths, mask, position, columns, rec, att, arrived, *refs):
    totals, (out, scratch) = refs[:-2], refs[-2:]
    value = partial(widths, mask, position, columns, rec, att, totals, scratch)
    out[...] = (value.astype(F32) + arrived[...].astype(F32)).astype(out.dtype)


def close_body(parts, gain, own, *refs):
    arrived, out = refs[:-1], refs[-1]
    pieces = []
    for n in range(parts):
        pieces.append(arrived[n][...].astype(F32))
        for other in arrived[n + parts :: parts]:
            pieces[n] = pieces[n] + other[...].astype(F32)
    mixed = own[...] + jnp.concatenate(pieces, axis=1)
    scale = lax.rsqrt(jnp.mean(mixed * mixed, axis=1, keepdims=True) + EPS)
    out[...] = (mixed * scale * gain[...]).astype(BF16)


def shards(
    tokens,
    pre_gain,
    rate_factor,
    w_rec_in,
    w_rec_gate,
    conv_taps,
    rate_maps,
    input_maps,
    decay_param,
    w_query,
    w_latent,
    w_rope_key,
    latent_gain,
    w_expand,
    rec_gain,
    att_gain,
    w_out_rec,
    w_out_att,
    post_gain,
):
    rows, depth = tokens.shape
    model_width, channels = w_rec_in.shape
    heads = w_query.shape[1] // (NOPE + ROPE)
    span = w_latent.shape[1]
    group = lax.axis_size("tp")
    chain = lax.axis_size("sp")
    place = lax.axis_index("sp")
    shape = jax.ShapeDtypeStruct
    half = rows // 2

    frequency = 1.0 / THETA ** (jnp.arange(0, ROPE, 2).astype(F32) / ROPE)
    places = (place * rows + jnp.arange(rows)).astype(F32)
    angle = places[:, None] * frequency[None, :]
    cosine, sine = jnp.cos(angle), jnp.sin(angle)
    decay = jax.nn.softplus(-decay_param)[None, :]

    chunks = 2
    width = depth // chunks
    *cut, ending = kernel(
        split_body,
        out_shape=[shape((rows, width), BF16)] * chunks + [shape((8, depth), BF16)],
        in_specs=[HBM],
        out_specs=[VMEM] * (chunks + 1),
        scratch_shapes=[pltpu.SemaphoreType.DMA((chunks + 1,))],
        compiler_params=params(4),
        cost_estimate=cost(1000000),
    )(in_hbm(tokens))
    side = {}
    for n in range(chunks):
        for m in range(2, group, 2):
            side[m, n] = swap(cut[n], "tp", m)
    twin = swap(tokens, "tp", 1)
    devices = range(chain)
    route = [(i, i + 1) for i in devices if i + 1 < chain]
    edge = {0: lax.ppermute(ending, "sp", route)}
    edge[1] = swap(edge[0], "tp", 1)
    for m in range(2, group, 2):
        edge[m] = swap(edge[0], "tp", m)
        edge[m + 1] = swap(edge[m], "tp", 1)
        for n in range(chunks):
            side[m + 1, n] = swap(side[m, n], "tp", 1)

    weights = [in_hbm(w) for w in (w_rec_in, w_rec_gate, w_query, w_latent, w_rope_key.T)]
    widths = [channels, channels, w_query.shape[1], span, ROPE]
    gain = pre_gain.reshape(group, 1, depth)
    partials = [shape((rows, w), F32) for w in widths]
    partials += [shape((rows, 1), F32), shape((8, channels), F32), shape((8, 1), F32)]
    finals = [
        shape((rows, channels), BF16),
        shape((8, channels), BF16),
        shape((rows, channels), F32),
        shape((heads, rows, NOPE + ROPE), BF16),
        shape((rows, span + ROPE), BF16),
        shape((half, span + ROPE), BF16),
    ]

    def buffers(count, size):
        sizes = [(count, size, w) for w in widths[:4]] + [(count, ROPE, size)]
        return sizes

    def project(places, blocks, held, sums, ahead, extra):
        size = blocks[0].shape[1]
        count = len(places)
        operands = [*blocks, *[edge[m] for m, _ in places], gain, *held, *sums, *extra]
        spaces = [VMEM] * (2 * count + 1) + [HBM if ahead else VMEM] * 5
        spaces += [VMEM] * (len(sums) + len(extra))
        outs, scratch = list(finals if extra else partials), []
        moved = 0
        if ahead:
            scratch = [pltpu.VMEM(b, BF16) for b in buffers(count, size)]
            scratch += [pltpu.SemaphoreType.DMA((1 + len(ahead), group, 5))]
            for some, wide in ahead:
                outs += [shape(b, BF16) for b in buffers(len(some), wide)]
            moved = 2 * model_width * sum(widths)
        return kernel(
            functools.partial(project_body, places, ahead, bool(extra)),
            out_shape=outs,
            in_specs=spaces,
            out_specs=[VMEM] * len(outs),
            scratch_shapes=scratch,
            compiler_params=params(16),
            cost_estimate=cost(2 * rows * size * count * sum(widths), moved),
        )(*operands)

    later = [[(m, n * width) for m in range(2, group)] for n in range(chunks)]
    ahead = [(some, width) for some in later]
    sums = project([(0, 0), (1, 0)], [tokens, twin], weights, [], ahead, [])
    sums, held = sums[:8], sums[8:]
    for n in range(chunks):
        extra = [cosine, sine, latent_gain[None, :]] if n == chunks - 1 else []
        blocks = [side[m, n] for m in range(2, group)]
        sums = project(later[n], blocks, held[5 * n : 5 * n + 5], sums, None, extra)
    rec_input, tail, gate_value, query, latent, mine = sums

    reached = {}
    for m in range(2, chain, 2):
        reached[m] = swap(mine, "sp", m)
    reached[1] = swap(mine, "sp", 1)
    for m in range(2, chain, 2):
        reached[m + 1] = swap(reached[m], "sp", 1)
    others = {m: swap(reached[m], "tp", 1) for m in reached}

    local, cum, whole = kernel(
        recur_body,
        out_shape=[
            shape((rows, channels), F32),
            shape((rows, channels), F32),
            shape((8, channels), F32),
        ],
        in_specs=[VMEM] * 7,
        out_specs=[VMEM] * 3,
        compiler_params=params(16),
        cost_estimate=cost(2 * rows * channels * 2000),
    )(rec_input, tail, conv_taps, rate_maps, input_maps, decay, rate_factor[None, :])
    reach = 1
    prefix = []
    while reach < chain // 2:
        theirs = swap(whole, "sp", reach)
        whole, before = kernel(
        functools.partial(pass_on_body, reach),
            out_shape=[shape((8, channels), F32)] * 2,
            in_specs=[VMEM] * (2 + len(prefix)),
            out_specs=[VMEM] * 2,
            compiler_params=params(4),
            cost_estimate=cost(200000),
        )(whole, theirs, *prefix)
        prefix = [before]
        reach *= 2
    theirs = swap(whole, "sp", reach)
    rec_out, rec_squares = kernel(
        functools.partial(finish_recur_body, reach),
        out_shape=[shape((rows, channels), F32), shape((8, rows), F32)],
        in_specs=[VMEM] * (4 + len(prefix)),
        out_specs=[VMEM] * 2,
        compiler_params=params(8),
        cost_estimate=cost(2 * rows * channels * 500),
    )(local, cum, gate_value, theirs, *prefix)

    rounds = [[0]]
    even = list(range(2, chain, 2))
    rounds.append([1] + even)
    odd = [m + 1 for m in even]
    rounds.append(odd[:-1])
    rounds.append(odd[-1:])
    state = []
    states = [shape((heads, rows, 128), F32)] * 3
    for n, masks in enumerate(rounds):
        final = n == len(rounds) - 1
        fetch = n == 1
        keys = []
        for m in masks:
            keys += [reached[m], others[m]] if m else [latent]
        operands = [query, *keys, w_expand, *state]
        spaces = [VMEM] * (len(operands))
        outs = states
        scratch = []
        if fetch:
            operands += [in_hbm(w_out_rec), in_hbm(w_out_att)]
            spaces += [HBM] * 2
            outs = states + [shape(w_out_rec.shape, BF16), shape(w_out_att.shape, BF16)]
            scratch = [pltpu.SemaphoreType.DMA((2,))]
        if final:
            operands += [rec_squares]
            spaces += [VMEM]
            outs = [shape((rows, heads * VDIM), F32), shape((16, rows), F32)]
        state = kernel(
            functools.partial(attend_body, masks, len(state), fetch, final),
            out_shape=outs,
            in_specs=spaces,
            out_specs=[VMEM] * len(outs),
            scratch_shapes=scratch,
            compiler_params=params(16),
            cost_estimate=cost(len(masks) * 2000 * rows * rows * 2),
        )(*operands)
        if fetch:
            w_rec_here, w_att_here = state[3:]
            state = state[:3]
    att_out, squares = state
    totals = [squares] + [swap(squares, "tp", m) for m in range(1, group)]

    size = rows // group
    rec_part, att_part = kernel(
        merge_body,
        out_shape=[shape((rows, model_width), F32)] * 2,
        in_specs=[VMEM] * 6,
        out_specs=[VMEM] * 2,
        scratch_shapes=[
            pltpu.VMEM((rows, channels), BF16),
            pltpu.VMEM((rows, heads * VDIM), BF16),
        ],
        compiler_params=params(24),
        cost_estimate=cost(2 * rows * (channels + heads * VDIM) * model_width),
    )(rec_out, att_out, rec_gain[None, :], att_gain[None, :], w_rec_here, w_att_here)
    norm_widths = (channels * group, heads * VDIM * group)
    split = 2
    width = model_width // split

    def part(body, mask, position, first, count, dtype, *more):
        columns = slice(first, first + count)
        return kernel(
        functools.partial(body, norm_widths, mask, position, columns),
            out_shape=shape((size, count), dtype),
            in_specs=[VMEM] * (2 + len(more) + len(totals)),
            out_specs=VMEM,
            scratch_shapes=[pltpu.VMEM((2, rows, 128), F32)],
            compiler_params=params(8),
            cost_estimate=cost(size * count * 200),
        )(rec_part, att_part, *more, *totals)

    arrivals = []
    for n in range(1, group // 2):
        for c in range(split):
            sent = part(send_body, 1 ^ (2 * n), n, c * width, width, BF16)
            came = swap(sent, "tp", 1)
            chip = part(chip_body, 2 * n, group // 2 + n, c * width, width, BF16, came)
            arrivals.append(swap(chip, "tp", 2 * n))
    sent = part(send_body, 1, 0, 0, model_width, BF16)
    came = swap(sent, "tp", 1)
    own = part(chip_body, 0, group // 2, 0, model_width, F32, came)
    return kernel(
        functools.partial(close_body, split),
        out_shape=shape((size, model_width), BF16),
        in_specs=[VMEM] * (2 + len(arrivals)),
        out_specs=VMEM,
        compiler_params=params(8),
        cost_estimate=cost(size * model_width * 100),
    )(post_gain[None, :], own, *arrivals)


def solution(mesh):
    placed = (
        P("sp", "tp"),
        P(),
        P("sp"),
        P(None, "tp"),
        P(None, "tp"),
        P(None, "tp"),
        P("tp", None, None),
        P("tp", None, None),
        P("tp"),
        P(None, "tp"),
        P(),
        P(),
        P(),
        P(None, "tp"),
        P("tp"),
        P("tp"),
        P("tp", None),
        P("tp", None),
        P(),
    )
    return jax.shard_map(
        shards, mesh=mesh, in_specs=placed, out_specs=P(("sp", "tp"), None), check_vma=False
    )
```
